32 devices in a mesh: sp: 8 (over z, y), tp: 4 (over x, core).
Axes of the slice: x: 2, y: 2, z: 4, core: 2. Of those that a mesh axis runs over, the one named last changes fastest.
Arguments:
- queries_nope: bfloat16 [3072, 8, 128], P('sp', 'tp'), may hold values from -9 to 9
- queries_rope: bfloat16 [3072, 8, 64], P('sp', 'tp'), may hold values from -6 to 6
- latent: bfloat16 [3072, 512], P('sp'), may hold values from -8 to 8, as said below
- rope_key: bfloat16 [3072, 64], P('sp'), may hold values from -6 to 6
- latent_gain: float32 [512], replicated, may hold values from 0.1 to 1.9
- key_up: bfloat16 [512, 1024], P(None, 'tp'), may hold values from -0.25 to 0.25
- value_up: bfloat16 [512, 1024], P(None, 'tp'), may hold values from -0.25 to 0.25
- out_proj: bfloat16 [1024, 2048], P('tp'), may hold values from -0.75 to 0.75
- stream: bfloat16 [3072, 2048], P(('sp', 'tp')), may hold values from -6 to 6
- mix_gain: float32 [2048], replicated, may hold values from 0.1 to 1.9
- w_gate: bfloat16 [2048, 3072], P('sp', 'tp'), may hold values from -0.125 to 0.125
- w_up: bfloat16 [2048, 3072], P('sp', 'tp'), may hold values from -0.125 to 0.125
- w_down: bfloat16 [3072, 2048], P('tp', 'sp'), may hold values from -0.4375 to 0.4375
- mlp_gain: float32 [2048], replicated, may hold values from 0.1 to 1.9
Outputs:
- result: bfloat16 [3072, 2048], P(('sp', 'tp'))
The draws below stay inside these ranges and needn't reach their ends.
Inputs may be any that keep to these rules, and one draw needn't show every extreme that they name: latent rows carry a mean vector that changes from one eighth of the sequence to the next.
All inputs are finite; a program needn't handle non-finite values.
Results may differ from the reference program's by a relative error of at most 0.017.
Values may be sent and summed in bfloat16 or wider, within the bound.
No kernel may reach another device: no remote copies, remote signals or barrier semaphores. Data moves between devices by JAX's collectives and lax.ppermute only.
A program may use at most 192 MiB of HBM per device.

```python
import math
import jax
import jax.numpy as jnp
from jax import lax

D = 2048
HEADS = 8
HEAD = 128
ROPE = 64
LATENT = 512
FF = 3072
SEQ = 3072


def draw_latent(key, part):
    base = jax.random.fold_in(key, 11)
    noise_key, centre_key, factor_key = jax.random.split(base, 3)
    places = jnp.arange(SEQ, dtype=jnp.int32)
    segment = places * 8 // SEQ
    centres = jax.random.normal(centre_key, (8, LATENT), jnp.float32) * 1.5
    noise = jax.random.normal(noise_key, (SEQ, LATENT), jnp.float32)
    return jnp.clip(noise + centres[segment], -8.0, 8.0).astype(jnp.bfloat16)


def rope_pair(key):
    base = jax.random.fold_in(key, 23)
    first_key, second_key, third_key = jax.random.split(base, 3)
    key_part = jnp.clip(jax.random.normal(first_key, (SEQ, ROPE), jnp.float32), -6.0, 6.0)
    query_part = jnp.clip(jax.random.normal(second_key, (SEQ, HEADS, ROPE), jnp.float32), -6.0, 6.0)
    return (query_part.astype(jnp.bfloat16), key_part.astype(jnp.bfloat16))


def draw_queries_rope(key, part):
    return rope_pair(key)[0]


def draw_rope_key(key, part):
    return rope_pair(key)[1]


def levels(own_key, dims, cuts, least, high):
    def one(dim, shards_of):
        heights = jax.random.uniform(jax.random.fold_in(jax.random.fold_in(own_key, 6), dim), (shards_of,), jnp.float32, least / len(cuts), high / len(cuts))
        return jnp.repeat(jnp.exp(heights), dims[dim] // shards_of).reshape((-1,) + (1,) * (len(dims) - dim - 1))

    factor_of = one(*cuts[0])
    for cut in cuts[1:]:
        factor_of = factor_of * one(*cut)
    return factor_of


def normal_values(own_key, dims, scale, reach, shards=(), held_as=jnp.bfloat16):
    loudness = levels(own_key, dims, shards, -0.22, 0.18) if shards else 1.0
    drawn = jax.random.normal(own_key, dims, jnp.float32) * scale * loudness
    return jnp.minimum(jnp.maximum(drawn, -reach), reach).astype(held_as)


def setup_inputs(seed: int = 0) -> dict:
    seeds = jax.random.split(jax.random.key(seed), 15)
    queries_nope = normal_values(seeds[0], (SEQ, HEADS, HEAD), 3.0, 9.0, ((0, 8), (1, 4)))
    queries_rope = draw_queries_rope(jax.random.fold_in(seeds[14], 71), 0)
    latent = draw_latent(jax.random.fold_in(seeds[14], 71), 0)
    rope_key = draw_rope_key(jax.random.fold_in(seeds[14], 71), 0)
    latent_gain = jnp.clip(1.0 + 0.18 * jax.random.normal(seeds[4], (LATENT,), jnp.float32), 0.1, 1.9)
    key_up = normal_values(seeds[5], (LATENT, HEADS * HEAD), LATENT ** -0.5, 0.25, ((1, 4),))
    value_up = normal_values(seeds[6], (LATENT, HEADS * HEAD), LATENT ** -0.5, 0.25, ((1, 4),))
    out_proj = normal_values(seeds[7], (HEADS * HEAD, D), (HEADS * HEAD // 16) ** -0.5, 0.75, ((0, 4),))
    stream = normal_values(seeds[8], (SEQ, D), 1.0, 6.0, ((0, 32),))
    mix_gain = jnp.clip(1.0 + 0.18 * jax.random.normal(seeds[9], (D,), jnp.float32), 0.1, 1.9)
    w_gate = normal_values(seeds[10], (D, FF), D ** -0.5, 0.125, ((0, 8), (1, 4)))
    w_up = normal_values(seeds[11], (D, FF), D ** -0.5, 0.125, ((0, 8), (1, 4)))
    w_down = normal_values(seeds[12], (FF, D), (FF // 16) ** -0.5, 0.4375, ((0, 4), (1, 8)))
    mlp_gain = jnp.clip(1.0 + 0.18 * jax.random.normal(seeds[13], (D,), jnp.float32), 0.1, 1.9)
    return dict(queries_nope=queries_nope, queries_rope=queries_rope, latent=latent, rope_key=rope_key, latent_gain=latent_gain, key_up=key_up, value_up=value_up, out_proj=out_proj, stream=stream, mix_gain=mix_gain, w_gate=w_gate, w_up=w_up, w_down=w_down, mlp_gain=mlp_gain)


theta_base = 10000.0
residual_weight = 8.0 ** 0.25
norm_floor = 1.0
big_negative = -1e+30

def rotate(vector, first_row):
    half = vector.shape[-1] // 2
    rates = theta_base ** (-2.0 * jnp.arange(half, dtype=jnp.float32) / vector.shape[-1])
    places = (first_row + jnp.arange(vector.shape[0], dtype=jnp.int32)).astype(jnp.float32)
    angle = places[:, None] * rates[None, :]
    angle = angle.reshape((vector.shape[0],) + (1,) * (vector.ndim - 2) + (half,))
    cosine = jnp.cos(angle)
    sine = jnp.sin(angle)
    left = vector[..., :half]
    right = vector[..., half:]
    return jnp.concatenate([left * cosine - right * sine, left * sine + right * cosine], axis=-1)

def latent_norm(latent, latent_gain):
    wide = latent.astype(jnp.float32)
    factor = lax.rsqrt(lax.optimization_barrier(jnp.mean(wide * wide, axis=-1, keepdims=True)) + norm_floor)
    return (wide * factor * latent_gain).astype(jnp.bfloat16)

def layer_norm(values, gain):
    centre = lax.optimization_barrier(jnp.mean(values, axis=-1, keepdims=True))
    centred = values - centre
    spread = lax.optimization_barrier(jnp.mean(centred * centred, axis=-1, keepdims=True))
    return centred * lax.rsqrt(spread + norm_floor) * gain

def widen(array):
    return lax.optimization_barrier(array).astype(jnp.float32)

def reference(queries_nope, queries_rope, latent, rope_key, latent_gain, key_up, value_up, out_proj, stream, mix_gain, w_gate, w_up, w_down, mlp_gain):
    seq_len, head_count, head_dim = queries_nope.shape
    rope_dim = queries_rope.shape[2]
    query_turned = rotate(queries_rope.astype(jnp.float32), 0).astype(jnp.bfloat16)
    key_turned = rotate(rope_key.astype(jnp.float32), 0).astype(jnp.bfloat16)
    normed = latent_norm(latent, latent_gain)
    keys = jnp.dot(normed, key_up, preferred_element_type=jnp.float32).astype(jnp.bfloat16)
    keys = widen(keys).reshape(seq_len, head_count, head_dim)
    values_all = jnp.dot(normed, value_up, preferred_element_type=jnp.float32).astype(jnp.bfloat16)
    values_all = widen(values_all).reshape(seq_len, head_count, head_dim)
    key_wide = key_turned.astype(jnp.float32)
    scale = (head_dim + rope_dim) ** (-0.5)
    block = math.gcd(seq_len, 512)
    key_places = jnp.arange(seq_len, dtype=jnp.int32)

    def one_block(index):
        begin = (index * block).astype(jnp.int32)
        query_block = lax.dynamic_slice_in_dim(queries_nope, begin, block, 0).astype(jnp.float32)
        turned_block = lax.dynamic_slice_in_dim(query_turned, begin, block, 0).astype(jnp.float32)
        score = jnp.einsum('thd,shd->hts', query_block, keys) + jnp.einsum('thr,sr->hts', turned_block, key_wide)
        score = score * scale
        allowed = key_places[None, :] <= (begin + jnp.arange(block, dtype=jnp.int32))[:, None]
        score = jnp.where(allowed[None], score, big_negative)
        top = lax.optimization_barrier(jnp.max(score, axis=2, keepdims=True))
        powers = jnp.exp(score - top) * allowed[None]
        denominators = lax.optimization_barrier(jnp.sum(powers, axis=2))
        summed = jnp.einsum('hts,shd->thd', widen(powers.astype(jnp.bfloat16)), values_all)
        return (summed / denominators.T[:, :, None]).astype(jnp.bfloat16)
    blocks = lax.map(one_block, jnp.arange(seq_len // block, dtype=jnp.int32))
    attended = blocks.reshape(seq_len, head_count * head_dim)
    projected = jnp.dot(attended, out_proj, preferred_element_type=jnp.float32)
    mixed = layer_norm(residual_weight * stream.astype(jnp.float32) + projected, mix_gain).astype(jnp.bfloat16)
    gate_sum = jnp.dot(mixed, w_gate, preferred_element_type=jnp.float32)
    up_sum = jnp.dot(mixed, w_up, preferred_element_type=jnp.float32)
    hidden = (jax.nn.silu(gate_sum) * up_sum).astype(jnp.bfloat16)
    lowered = jnp.dot(hidden, w_down, preferred_element_type=jnp.float32)
    return layer_norm(residual_weight * mixed.astype(jnp.float32) + 0.5 * lowered, mlp_gain).astype(jnp.bfloat16)
```

```python
import jax
import jax.numpy as jnp
from jax import lax
from jax.sharding import PartitionSpec as P

theta_base = 10000.0
residual_weight = 8.0**0.25
norm_floor = 1.0
big_negative = -1e30


def rotate(vector, first_row):
    half = vector.shape[-1] // 2
    rates = theta_base ** (-2.0 * jnp.arange(half, dtype=jnp.float32) / vector.shape[-1])
    places = (first_row + jnp.arange(vector.shape[0], dtype=jnp.int32)).astype(jnp.float32)
    angle = places[:, None] * rates[None, :]
    angle = angle.reshape((vector.shape[0],) + (1,) * (vector.ndim - 2) + (half,))
    cosine = jnp.cos(angle)
    sine = jnp.sin(angle)
    left = vector[..., :half]
    right = vector[..., half:]
    return jnp.concatenate([left * cosine - right * sine, left * sine + right * cosine], axis=-1)


def latent_norm(latent, latent_gain):
    wide = latent.astype(jnp.float32)
    factor = lax.rsqrt(jnp.mean(wide * wide, axis=-1, keepdims=True) + norm_floor)
    return (wide * factor * latent_gain).astype(jnp.bfloat16)


def layer_norm(values, gain):
    centre = jnp.mean(values, axis=-1, keepdims=True)
    centred = values - centre
    spread = jnp.mean(centred * centred, axis=-1, keepdims=True)
    return centred * lax.rsqrt(spread + norm_floor) * gain


pair = 2
axes = ("sp", "tp")


def make_perm(sp_count, tp_count, move):
    out = []
    for sp in range(sp_count):
        for tp in range(tp_count):
            where = move(sp // pair, sp % pair, tp // pair, tp % pair)
            if where is not None:
                z, y, x, c = where
                out.append((sp * tp_count + tp, (z * pair + y) * tp_count + x * pair + c))
    return out


class Moves:
    def __init__(self, sp_count, tp_count):
        self.z_count = sp_count // pair
        self.counts = (sp_count, tp_count)
        self.z = lax.axis_index("sp") // pair
        self.y = lax.axis_index("sp") % pair
        self.x = lax.axis_index("tp") // pair
        self.c = lax.axis_index("tp") % pair

    def go(self, value, move):
        return lax.ppermute(value, axes, make_perm(*self.counts, move))

    def flip_y(self, value):
        return self.go(value, lambda z, y, x, c: (z, 1 - y, x, c))

    def flip_x(self, value):
        return self.go(value, lambda z, y, x, c: (z, y, x ^ 1, c))

    def flip_c(self, value):
        return self.go(value, lambda z, y, x, c: (z, y, x, 1 - c))

    def shift_z(self, value, by):
        last = self.z_count
        return self.go(value, lambda z, y, x, c: (z + by, y, x, c) if 0 <= z + by < last else None)

    def plane_gather(self, own):
        half = own.shape[0] // 2
        from_x = self.flip_x(own)
        from_y = self.flip_y(own)
        corner = jnp.concatenate(
            [self.flip_x(from_y[:half]), self.flip_y(from_x[half:])], axis=0
        )
        near = jnp.stack([own, from_x, from_y])
        far_near = self.flip_c(near)
        far_corner = self.flip_c(corner)
        mine = jnp.concatenate([near, corner[None]], axis=0)
        other = jnp.concatenate([far_near, far_corner[None]], axis=0)
        both = jnp.stack([mine, other], axis=1)
        return both.reshape((pair, pair, pair) + own.shape)

    def plane_scatter(self, terms):
        low = jnp.bfloat16
        got = self.flip_c(terms[:, :, 1].astype(low))
        sums = terms[:, :, 0] + got.astype(jnp.float32)
        sent = sums.astype(low)
        half = sent.shape[2] // 2
        via_x = self.flip_x(jnp.concatenate([sent[0, 1], sent[1, 1, :half]], axis=0))
        via_y = self.flip_y(jnp.concatenate([sent[1, 0], sent[1, 1, half:]], axis=0))
        rows = sent.shape[2]
        tail_y = self.flip_y(via_x[rows:])
        tail_x = self.flip_x(via_y[rows:])
        wide = [v.astype(jnp.float32) for v in (via_x[:rows], via_y[:rows])]
        corner = jnp.concatenate([tail_y, tail_x], axis=0).astype(jnp.float32)
        return sums[0, 0] + wide[0] + wide[1] + corner

    def line_gather(self, own):
        count = self.z_count
        from_left = [own]
        from_right = [own]
        for _ in range(count - 1):
            from_left.append(self.shift_z(from_left[-1], 1))
            from_right.append(self.shift_z(from_right[-1], -1))
        orders = []
        for z in range(count):
            order = []
            for step in range(1, count):
                if z + step < count:
                    order.append((step, 1))
                if z - step >= 0:
                    order.append((step, -1))
            orders.append(order)
        pieces = [(own, self.z)]
        for item in range(count - 1):
            wanted = [orders[z][item] for z in range(count)]
            value = None
            for choice in sorted(set(wanted)):
                step, side = choice
                here = (from_right if side == 1 else from_left)[step]
                if value is None:
                    value = here
                else:
                    flags = jnp.array([w == choice for w in wanted])
                    value = jnp.where(flags[self.z], here, value)
            steps = jnp.array([step * side for step, side in wanted], dtype=jnp.int32)
            pieces.append((value, self.z + steps[self.z]))
        return pieces


def per_device(
    queries_nope,
    queries_rope,
    latent,
    rope_key,
    latent_gain,
    key_up,
    value_up,
    out_proj,
    stream,
    mix_gain,
    w_gate,
    w_up,
    w_down,
    mlp_gain,
    sp_count,
    tp_count,
):
    grid = Moves(sp_count, tp_count)
    row_count, head_count, head_dim = queries_nope.shape
    rope_dim = queries_rope.shape[2]
    latent_dim = latent.shape[1]
    quarter = stream.shape[0]
    width = stream.shape[1]
    first_row = lax.axis_index("sp") * row_count

    hidden_half = w_gate.shape[1] // pair

    def take(array, index, axis):
        return lax.dynamic_slice_in_dim(array, index * hidden_half, hidden_half, axis)

    def gate_up(index):
        return jnp.concatenate([take(w_gate, index, 1), take(w_up, index, 1)], axis=1)

    def ordered(own, partner, axis):
        first = jnp.where(grid.y == 0, own, partner)
        second = jnp.where(grid.y == 0, partner, own)
        return jnp.concatenate([first, second], axis=axis)

    key_turned = rotate(rope_key.astype(jnp.float32), first_row).astype(jnp.bfloat16)
    normed = latent_norm(latent, latent_gain)
    packed = jnp.concatenate([normed, key_turned], axis=1)
    mine = lax.dynamic_slice_in_dim(packed, lax.axis_index("tp") * quarter, quarter, 0)
    earlier = [grid.shift_z(mine, step) for step in range(1, grid.z_count)]

    gu_partner = grid.flip_y(gate_up(1 - grid.y))
    gu_own = ordered(gate_up(grid.y), gu_partner, 0)

    def relative_places(block_z):
        dy, dx, dc, row = jnp.meshgrid(
            jnp.arange(pair), jnp.arange(pair), jnp.arange(pair), jnp.arange(quarter), indexing="ij"
        )
        block = block_z * pair + (grid.y + dy) % pair
        part = ((grid.x ^ dx) * pair) + (grid.c + dc) % pair
        return (block * row_count + part * quarter + row).astype(jnp.int32)

    near_y = grid.flip_y(mine)
    near_yx = grid.flip_x(near_y)
    near = jnp.stack([near_y, near_yx])
    near_far = grid.flip_c(near)
    neighbour = jnp.stack([near, near_far], axis=1)
    key_parts = [packed, neighbour.reshape(-1, packed.shape[1])]
    key_places = [
        first_row + jnp.arange(row_count, dtype=jnp.int32),
        relative_places(grid.z)[1].reshape(-1),
    ]
    groups = [list(range(1, grid.z_count))[:1], list(range(1, grid.z_count))[1:]]
    for group in groups:
        if not group:
            continue
        stacked = jnp.stack([earlier[step - 1] for step in group], axis=1)
        gathered = grid.plane_gather(stacked)
        key_parts.append(jnp.moveaxis(gathered, 4, 3).reshape(-1, packed.shape[1]))
        places = jnp.stack([relative_places(grid.z - step) for step in group], axis=3)
        key_places.append(places.reshape(-1))
    all_packed = jnp.concatenate(key_parts, axis=0)
    all_places = jnp.concatenate(key_places, axis=0)

    gu_own, last_earlier = lax.optimization_barrier((gu_own, earlier[-1]))
    gu_pieces = grid.line_gather(gu_own)
    all_packed, out_proj, w_down = lax.optimization_barrier((all_packed, out_proj, w_down))
    proj_x = grid.flip_x(out_proj)
    proj_near = jnp.stack([out_proj, proj_x])
    down_partner = grid.flip_y(take(w_down, 1 - grid.y, 0))
    down_own = ordered(take(w_down, grid.y, 0), down_partner, 1)
    down_pieces = grid.line_gather(down_own)
    proj_far = grid.flip_c(proj_near)
    whole_proj = jnp.stack([proj_near, proj_far], axis=1).reshape(-1, width)

    query_turned = rotate(queries_rope.astype(jnp.float32), first_row).astype(jnp.bfloat16)
    scale = (head_dim + rope_dim) ** (-0.5)
    query_places = first_row + jnp.arange(row_count, dtype=jnp.int32)
    latent_all = all_packed[:, :latent_dim]
    rotary_all = all_packed[:, latent_dim:]
    count = latent_all.shape[0]
    keys = jnp.dot(latent_all, key_up, preferred_element_type=jnp.float32).astype(jnp.bfloat16)
    keys = keys.reshape(count, head_count, head_dim)
    values_here = jnp.dot(latent_all, value_up, preferred_element_type=jnp.float32)
    values_here = values_here.astype(jnp.bfloat16).reshape(count, head_count, head_dim)
    score = jnp.einsum("thd,shd->hts", queries_nope, keys, preferred_element_type=jnp.float32)
    score = score + jnp.einsum(
        "thr,sr->hts", query_turned, rotary_all, preferred_element_type=jnp.float32
    )
    score = score * scale
    allowed = (all_places[None, :] <= query_places[:, None]) & (all_places >= 0)[None, :]
    score = jnp.where(allowed[None], score, big_negative)
    top = jnp.max(score, axis=2, keepdims=True)
    powers = jnp.exp(score - top) * allowed[None]
    denominators = jnp.sum(powers, axis=2)
    weighted = jnp.einsum(
        "hts,shd->thd",
        powers.astype(jnp.bfloat16),
        values_here,
        preferred_element_type=jnp.float32,
    )
    attended = (weighted / denominators.T[:, :, None]).astype(jnp.bfloat16)
    attended = attended.reshape(tp_count // pair, pair, quarter, head_count * head_dim)

    def pick(array, index, axis):
        return lax.dynamic_index_in_dim(array, index, axis, keepdims=False)

    if tp_count == pair * pair:
        got_x = grid.flip_x(pick(attended, 1 - grid.x, 0))
        by_x = jnp.stack([pick(attended, grid.x, 0), got_x])
        got_c = grid.flip_c(pick(by_x, 1 - grid.c, 1))
        row_heads = jnp.stack([pick(by_x, grid.c, 1), got_c], axis=1)
    row_heads = jnp.moveaxis(row_heads, 2, 0).reshape(quarter, -1)
    projected = jnp.dot(row_heads, whole_proj, preferred_element_type=jnp.float32)
    mixed = layer_norm(residual_weight * stream.astype(jnp.float32) + projected, mix_gain).astype(
        jnp.bfloat16
    )
    plane_rows = grid.plane_gather(mixed).reshape(-1, width)

    gu_all = jnp.zeros((width, 2 * hidden_half), jnp.bfloat16)
    for value, source in gu_pieces:
        gu_all = lax.dynamic_update_slice_in_dim(gu_all, value, source * value.shape[0], 0)
    sums = jnp.dot(plane_rows, gu_all, preferred_element_type=jnp.float32)
    hidden = (jax.nn.silu(sums[:, :hidden_half]) * sums[:, hidden_half:]).astype(jnp.bfloat16)

    lowered = jnp.zeros((quarter, width), jnp.float32)
    split = max(1, len(down_pieces) - 2)
    for piece_group in (down_pieces[:split], down_pieces[split:-1], down_pieces[-1:]):
        if not piece_group:
            continue
        weights = jnp.concatenate([value for value, _ in piece_group], axis=1)
        terms = jnp.dot(hidden, weights, preferred_element_type=jnp.float32)
        done = grid.plane_scatter(terms.reshape(pair, pair, pair, quarter, -1))
        span = piece_group[0][0].shape[1]
        for index, (_, source) in enumerate(piece_group):
            part = done[:, index * span : (index + 1) * span]
            lowered = lax.dynamic_update_slice_in_dim(lowered, part, source * span, 1)
    return layer_norm(residual_weight * mixed.astype(jnp.float32) + 0.5 * lowered, mlp_gain).astype(
        jnp.bfloat16
    )


def solution(mesh):
    sp_count = mesh.shape["sp"]
    tp_count = mesh.shape["tp"]
    return jax.shard_map(
        lambda *arrays: per_device(*arrays, sp_count=sp_count, tp_count=tp_count),
        mesh=mesh,
        in_specs=(
            P("sp", "tp", None),
            P("sp", "tp", None),
            P("sp", None),
            P("sp", None),
            P(),
            P(None, "tp"),
            P(None, "tp"),
            P("tp", None),
            P(("sp", "tp"), None),
            P(),
            P("sp", "tp"),
            P("sp", "tp"),
            P("tp", "sp"),
            P(),
        ),
        out_specs=P(("sp", "tp"), None),
        check_vma=False,
    )
```
